32 devices in a mesh: sp: 16 (over z, y, x), tp: 2 (over core).
Axes of the slice: x: 2, y: 2, z: 4, core: 2. Of those that a mesh axis runs over, the one named last changes fastest.
Arguments:
- latent: bfloat16 [4096, 2048], P(('sp', 'tp')), may hold values from -6 to 6
- condition: bfloat16 [2048], P('sp'), may hold values from -6 to 6
- context_condition: bfloat16 [2048], P('sp'), may hold values from -6 to 6
- context: bfloat16 [512, 2048], P('sp'), may hold values from -6 to 6
- w_shift: bfloat16 [2048, 2048], P('sp', 'tp'), may hold values from -0.125 to 0.125
- w_scale: bfloat16 [2048, 2048], P('sp', 'tp'), may hold values from -0.125 to 0.125
- w_gate: bfloat16 [2048, 2048], P('sp', 'tp'), may hold values from -0.125 to 0.125
- pre_gain: float32 [2048], replicated, may hold values from 0.1 to 1.9
- post_gain: float32 [2048], replicated, may hold values from 0.1 to 1.9
- query_gain: float32 [128], replicated, may hold values from 0.1 to 5
- key_gain: float32 [128], replicated, may hold values from 0.1 to 5
- w_query: bfloat16 [2048, 2048], P(None, 'tp'), may hold values from -0.125 to 0.125
- w_key: bfloat16 [2048, 1024], P(None, 'tp'), may hold values from -0.125 to 0.125
- w_value: bfloat16 [2048, 1024], P(None, 'tp'), may hold values from -0.125 to 0.125
- w_out: bfloat16 [2048, 2048], P('tp'), may hold values from -0.125 to 0.125
Outputs:
- updated: bfloat16 [4096, 2048], P(('sp', 'tp'))
The draws below stay inside these ranges and needn't reach their ends.
All inputs are finite; a program needn't handle non-finite values.
Results may differ from the reference program's by a relative error of at most 0.0085.
The reference program's roundings to bfloat16 on the way count: a program that leaves them out, or rounds other values in their place, can miss the bound.
Values may be sent and summed in bfloat16 or wider, within the bound.
A program may use at most 64 MiB of HBM per device.

```python
import math
import jax
import jax.numpy as jnp
from jax import lax

D = 2048
HEADS = 16
KV_HEADS = 8
HEAD_DIM = 128
GRID_W = 64
CTX = 512
TOKENS = 4096
N_TP = 2


def gain_draw(key):
    return 1.0 + 0.18 * jnp.clip(jax.random.normal(key, (HEAD_DIM,), jnp.float32), -4.5, 4.5)


def draw_query_gain(key, part):
    return gain_draw(jax.random.fold_in(key, 11))


def draw_key_gain(key, part):
    return gain_draw(jax.random.fold_in(key, 23))


def block_scale(key, extent, cuts, smallest, top_value):
    factor_of = 1.0
    for position, parts in cuts:
        steps = jax.random.uniform(jax.random.fold_in(jax.random.fold_in(key, 6), position), (parts,), jnp.float32, smallest / len(cuts), top_value / len(cuts))
        factor_of = factor_of * jnp.repeat(jnp.exp(steps), extent[position] // parts).reshape((-1,) + (1,) * (len(extent) - 1 - position))
    return factor_of


def gaussian(key, extent, deviation, bound, cuts=(), held_as=jnp.bfloat16):
    level = block_scale(key, extent, cuts, -0.22, 0.18) if cuts else 1.0
    drawn = jax.random.normal(key, extent, jnp.float32) * deviation * level
    return jnp.minimum(jnp.maximum(drawn, -bound), bound).astype(held_as)


def setup_inputs(seed: int = 0) -> dict:
    arg_keys = jax.random.split(jax.random.key(seed), 16)
    return {
        "latent": gaussian(arg_keys[0], (TOKENS, D), 1.0, 6.0, ((0, 32),)),
        "condition": gaussian(arg_keys[1], (D,), 1.0, 6.0, ((0, 16),)),
        "context_condition": gaussian(arg_keys[2], (D,), 1.0, 6.0, ((0, 16),)),
        "context": gaussian(arg_keys[3], (CTX, D), 1.0, 6.0, ((0, 16),)),
        "w_shift": gaussian(arg_keys[4], (D, D), D ** -0.5, 0.125, ((0, 16), (1, 2))),
        "w_scale": gaussian(arg_keys[5], (D, D), D ** -0.5, 0.125, ((0, 16), (1, 2))),
        "w_gate": gaussian(arg_keys[6], (D, D), D ** -0.5, 0.125, ((0, 16), (1, 2))),
        "pre_gain": jnp.clip(1.0 + 0.18 * jax.random.normal(arg_keys[7], (D,), jnp.float32), 0.1, 1.9),
        "post_gain": jnp.clip(1.0 + 0.18 * jax.random.normal(arg_keys[8], (D,), jnp.float32), 0.1, 1.9),
        "query_gain": draw_query_gain(jax.random.fold_in(arg_keys[15], 71), 0),
        "key_gain": draw_key_gain(jax.random.fold_in(arg_keys[15], 71), 0),
        "w_query": gaussian(arg_keys[11], (D, HEADS * HEAD_DIM), D ** -0.5, 0.125, ((1, 2),)),
        "w_key": gaussian(arg_keys[12], (D, KV_HEADS * HEAD_DIM), D ** -0.5, 0.125, ((1, 2),)),
        "w_value": gaussian(arg_keys[13], (D, KV_HEADS * HEAD_DIM), D ** -0.5, 0.125, ((1, 2),)),
        "w_out": gaussian(arg_keys[14], (HEADS * HEAD_DIM, D), (HEADS * HEAD_DIM) ** -0.5, 0.125, ((0, 2),)),
    }


def rms(values, gain):
    values = values.astype(jnp.float32)
    return values * lax.rsqrt(lax.optimization_barrier(jnp.mean(values * values, axis=-1, keepdims=True)) + 1e-06) * gain

def rotate_grid(values, positions, grid_width):
    head_dim = values.shape[-1]
    half = head_dim // 2
    quarter = head_dim // 4
    freqs = 10000.0 ** (-jnp.arange(0, half, 2).astype(jnp.float32) / half)
    row_pos = (positions // grid_width).astype(jnp.float32)
    col_pos = (positions % grid_width).astype(jnp.float32)
    pieces = []
    for axis_pos, base in ((row_pos, 0), (col_pos, half)):
        angle = axis_pos[:, None, None] * freqs
        cosine = jnp.cos(angle)
        sine = jnp.sin(angle)
        first = values[..., base:base + quarter]
        second = values[..., base + quarter:base + half]
        pieces = pieces + [first * cosine - second * sine, second * cosine + first * sine]
    return jnp.concatenate(pieces, axis=-1)

def reference(latent, condition, context_condition, context, w_shift, w_scale, w_gate, pre_gain, post_gain, query_gain, key_gain, w_query, w_key, w_value, w_out):
    head_dim = HEAD_DIM
    group = HEADS // KV_HEADS
    conds = jax.nn.silu(jnp.stack([condition, context_condition]).astype(jnp.float32)).astype(jnp.bfloat16)
    shift = jnp.dot(conds, w_shift, preferred_element_type=jnp.float32)
    scale = jnp.dot(conds, w_scale, preferred_element_type=jnp.float32)
    gate = jnp.dot(conds, w_gate, preferred_element_type=jnp.float32)
    normed = (rms(latent, pre_gain) * (1.0 + scale[0]) + shift[0]).astype(jnp.bfloat16)
    normed_context = (rms(context, pre_gain) * (1.0 + scale[1]) + shift[1]).astype(jnp.bfloat16)
    positions = jnp.arange(TOKENS).astype(jnp.int32)
    query = jnp.dot(normed, w_query, preferred_element_type=jnp.float32).reshape(TOKENS, HEADS, head_dim)
    query = rotate_grid(rms(query, query_gain), positions, GRID_W).astype(jnp.bfloat16)
    key = jnp.dot(normed, w_key, preferred_element_type=jnp.float32).reshape(TOKENS, KV_HEADS, head_dim)
    key = rotate_grid(rms(key, key_gain), positions, GRID_W).astype(jnp.bfloat16)
    value = jnp.dot(normed, w_value, preferred_element_type=jnp.float32).astype(jnp.bfloat16)
    value = value.reshape(TOKENS, KV_HEADS, head_dim)
    context_key = jnp.dot(normed_context, w_key, preferred_element_type=jnp.float32).reshape(CTX, KV_HEADS, head_dim)
    context_key = rms(context_key, key_gain).astype(jnp.bfloat16)
    context_value = jnp.dot(normed_context, w_value, preferred_element_type=jnp.float32).astype(jnp.bfloat16)
    context_value = context_value.reshape(CTX, KV_HEADS, head_dim)
    all_keys = jnp.concatenate([key, context_key], axis=0).astype(jnp.float32)
    all_values = jnp.concatenate([value, context_value], axis=0).astype(jnp.float32)
    lift = math.log(TOKENS / (4.0 * CTX))
    offsets = jnp.concatenate([jnp.zeros((TOKENS,), jnp.float32), jnp.full((CTX,), lift, jnp.float32)])
    block = 128
    blocked = query.reshape(TOKENS // block, block, KV_HEADS, group, head_dim)

    def one_block(query_block):
        scores = jnp.einsum('tkgd,skd->kgts', query_block.astype(jnp.float32), all_keys) * head_dim ** (-0.5)
        scores = scores + offsets
        largest = lax.optimization_barrier(jnp.max(scores, axis=-1, keepdims=True))
        terms = jnp.exp(scores - largest)
        total = lax.optimization_barrier(jnp.sum(terms, axis=-1))
        rounded = lax.optimization_barrier(terms.astype(jnp.bfloat16)).astype(jnp.float32)
        summed = jnp.einsum('kgts,skd->kgtd', rounded, all_values)
        result = summed / total[..., None]
        return result.transpose(2, 0, 1, 3).reshape(block, HEADS * head_dim).astype(jnp.bfloat16)
    attended = lax.map(one_block, blocked).reshape(TOKENS, HEADS * head_dim)
    group_width = HEADS * head_dim // N_TP
    mixed = jnp.zeros((TOKENS, D), jnp.float32)
    for index in range(N_TP):
        columns = attended[:, index * group_width:(index + 1) * group_width]
        rows_out = w_out[index * group_width:(index + 1) * group_width]
        partial_value = jnp.dot(columns, rows_out, preferred_element_type=jnp.float32).astype(jnp.bfloat16)
        mixed = mixed + lax.optimization_barrier(partial_value).astype(jnp.float32)
    updated = latent.astype(jnp.float32) + gate[0] * rms(mixed, post_gain)
    return updated.astype(jnp.bfloat16)
```

```python
import functools
import math

import jax
import jax.numpy as jnp
from jax import lax
from jax.experimental import pallas as pl
from jax.experimental.pallas import tpu as pltpu
from jax.sharding import PartitionSpec as P

GRID_W = 64
EPS = 1e-06
ONES = 16
F32 = jnp.float32
BF16 = jnp.bfloat16
MESH = pl.DeviceIdType.MESH


def kernel(
    sizes,
    latent,
    cond,
    ctx_cond,
    context,
    w_shift,
    w_scale,
    w_gate,
    pre_gain,
    post_gain,
    query_gain,
    key_gain,
    w_query,
    w_key,
    w_value,
    w_out,
    out,
    wq,
    wkv,
    wo,
    lat_all,
    lat_next,
    mod_part,
    mod_recv,
    gate_part,
    gate_recv,
    mod_all,
    gate_all,
    xn,
    kv_send,
    q_send,
    kvb,
    qb,
    m_ref,
    acc_ref,
    s0,
    s1,
    n0,
    n1,
    att_send,
    att_recv,
    psum,
    part_send,
    part_recv,
    w_sem,
    lat_ss,
    lat_rs,
    ln_ss,
    ln_rs,
    lz_ss,
    red_sem,
    ma_ss,
    ma_rs,
    ga_ss,
    ga_rs,
    kva_ss,
    kvz_ss,
    kv_rs,
    cx_ss,
    cx_rs,
    q_ss,
    q_rs,
    at_ss,
    at_rs,
    pt_ss,
    pt_rs,
):
    n_sp, n_tp, fan, planes, group, hd, tok, rows, ctx = sizes
    width = w_shift.shape[1]
    qw = group * hd
    wide = group * tok
    early = planes >= 4
    me = lax.axis_index("sp")
    mt = lax.axis_index("tp")
    if fan == 1:
        f, g = 0, me
    else:
        f, g = lax.rem(me, fan), lax.div(me, fan)
    top, bottom = g == planes - 1, g == 0
    edge = top | bottom
    beside = jnp.where(bottom, 1, planes - 2)

    def remote(src, dst, ss, rs, **where):
        return pltpu.make_async_remote_copy(
            src_ref=src, dst_ref=dst, send_sem=ss, recv_sem=rs, device_id=where, device_id_type=MESH
        )

    loads = [pltpu.make_async_copy(w_query, wq, w_sem.at[0])]
    kv_loads = []
    for i in range(fan):
        cols = pl.ds(i * hd, hd)
        kv_loads.append(
            pltpu.make_async_copy(w_key.at[:, cols], wkv.at[i, :, pl.ds(0, hd)], w_sem.at[2 + 2 * i])
        )
        kv_loads.append(
            pltpu.make_async_copy(
                w_value.at[:, cols], wkv.at[i, :, pl.ds(hd, hd)], w_sem.at[3 + 2 * i]
            )
        )
    out_load = pltpu.make_async_copy(w_out, wo, w_sem.at[1])
    for copy in kv_loads + loads + [out_load]:
        copy.start()

    bar = pltpu.get_barrier_semaphore()

    @pl.loop(1, n_sp)
    def _(d):
        pl.semaphore_signal(
            bar, inc=1, device_id={"sp": lax.rem(me + d, n_sp)}, device_id_type=MESH
        )

    for d in range(1, n_tp):
        pl.semaphore_signal(
            bar, inc=1, device_id={"tp": lax.rem(mt + d, n_tp)}, device_id_type=MESH
        )

    def silu(v):
        v = v.astype(F32)
        return v / (1.0 + jnp.exp(-v))

    row_id = lax.broadcasted_iota(jnp.int32, (8, cond.shape[1]), 0)
    conds = jnp.where(
        row_id == 0, silu(cond[...]), jnp.where(row_id == 1, silu(ctx_cond[...]), 0.0)
    ).astype(BF16)
    part_shift = jnp.dot(conds, w_shift[...], preferred_element_type=F32)
    part_scale = jnp.dot(conds, w_scale[...], preferred_element_type=F32)
    part_gate = jnp.dot(conds, w_gate[...], preferred_element_type=F32)
    mod_part[0:2, :] = part_shift[0:2]
    mod_part[2:4, :] = part_scale[0:2]
    gate_part[...] = part_gate[0:1]

    lane = lax.broadcasted_iota(jnp.int32, (tok, hd), 1)
    quarter = hd // 4
    low = (lane & quarter) == 0

    def turns(chip_index):
        pos = (chip_index * tok + lax.broadcasted_iota(jnp.int32, (tok, hd), 0)).astype(F32)
        row_pos = jnp.floor(pos * (1.0 / GRID_W))
        col_pos = pos - row_pos * GRID_W
        step = (lane & (quarter - 1)).astype(F32)
        freq = jnp.exp(step * (-2.0 * math.log(10000.0) / (hd // 2)))
        angle = jnp.where(lane < hd // 2, row_pos, col_pos) * freq
        sine = jnp.sin(angle)
        return jnp.cos(angle), jnp.where(low, -sine, sine)

    pl.semaphore_wait(bar, n_sp - 1 + n_tp - 1)

    def mod_copy(d, slot):
        peer = lax.rem(me + d, n_sp)
        return remote(mod_part, mod_recv.at[slot], red_sem.at[0], red_sem.at[1], sp=peer)

    def gate_copy(d, slot):
        peer = lax.rem(me + d, n_sp)
        return remote(gate_part, gate_recv.at[slot], red_sem.at[2], red_sem.at[3], sp=peer)

    def wait_all(ref, sem):
        most = ref.at[pl.ds(0, n_sp - 1)]
        pltpu.make_async_copy(most, most, sem).wait()

    @pl.loop(1, n_sp)
    def _(d):
        mod_copy(d, d - 1).start()

    def lat_copy(d, slot):
        peer = lax.rem(mt + d, n_tp)
        return remote(latent, lat_all.at[slot], lat_ss.at[d], lat_rs.at[slot], tp=peer)

    for d in range(1, n_tp):
        lat_copy(d, mt).start()

    @pl.loop(1, n_sp)
    def _(d):
        gate_copy(d, d - 1).start()

    def next_copy(way):
        peer = me + fan if way == 0 else me - fan
        return remote(latent, lat_next.at[mt], lz_ss.at[way], ln_rs.at[mt], sp=peer)

    send_up = early & (g == planes - 2)
    send_down = early & (g == 1)

    @pl.when(send_up)
    def _():
        next_copy(0).start()

    @pl.when(send_down)
    def _():
        next_copy(1).start()

    mod_recv[n_sp - 1] = mod_part[...]
    gate_recv[n_sp - 1] = gate_part[...]
    lat_all[mt] = latent[...]

    cosine, sine = turns(me)

    def head_rms(v, gain):
        return v * lax.rsqrt(jnp.mean(v * v, axis=-1, keepdims=True) + EPS) * gain

    def rotate(v, cosine, sine):
        other = jnp.where(low, pltpu.roll(v, hd - quarter, 1), pltpu.roll(v, quarter, 1))
        return v * cosine + other * sine

    for d in range(1, n_tp):
        lat_copy(d, lax.rem(mt + d, n_tp)).wait_recv()

    def inverse(v):
        return lax.rsqrt(jnp.mean(v * v, axis=-1, keepdims=True) + EPS)

    lat_inv = [inverse(lat_all[t].astype(F32)) for t in range(n_tp)]
    ctx_inv = inverse(context[...].astype(F32))
    m_ref[...] = jnp.full(m_ref.shape, -1e30, F32)
    acc_ref[...] = jnp.zeros(acc_ref.shape, F32)

    wait_all(mod_recv, red_sem.at[1])
    mod_all[mt] = lax.fori_loop(1, n_sp, lambda i, s: s + mod_recv[i], mod_recv[0])

    def ma_copy(d, slot):
        peer = lax.rem(mt + d, n_tp)
        return remote(mod_all.at[mt], mod_all.at[slot], ma_ss.at[d], ma_rs.at[slot], tp=peer)

    for d in range(1, n_tp):
        ma_copy(d, mt).start()
    for d in range(1, n_tp):
        ma_copy(d, lax.rem(mt + d, n_tp)).wait_recv()

    def modulate(latents, inverses):
        for t in range(n_tp):
            cols = slice(t * width, (t + 1) * width)
            scale0 = 1.0 + mod_all[t, 2:3]
            for s in range(n_tp):
                v = latents[s, :, cols].astype(F32) * inverses[s] * pre_gain[:, cols]
                xn[s * rows : (s + 1) * rows, cols] = (v * scale0 + mod_all[t, 0:1]).astype(BF16)

    modulate(lat_all, lat_inv)
    for t in range(n_tp):
        cols = slice(t * width, (t + 1) * width)
        v = context[:, cols].astype(F32) * ctx_inv * pre_gain[:, cols]
        xn[tok : tok + ctx, cols] = (v * (1.0 + mod_all[t, 3:4]) + mod_all[t, 1:2]).astype(BF16)

    for copy in kv_loads:
        copy.wait()

    def chip(plane, i):
        return plane * fan + i

    main = pl.ds(0, 2 * tok)
    extra = pl.ds(2 * tok, 2 * ctx)

    def put_kv(both, dst, cosine, sine):
        k = head_rms(both[:, :hd], key_gain[...])
        v = both[:, hd:]
        dst[0:tok] = rotate(k[:tok], cosine, sine).astype(BF16)
        for c in range(tok // hd):
            dst[tok + c * hd : tok + (c + 1) * hd] = v[c * hd : (c + 1) * hd].T.astype(BF16)
        if both.shape[0] > tok:
            dst[2 * tok : 2 * tok + ctx] = k[tok:].astype(BF16)
            dst[2 * tok + ctx : 2 * tok + 2 * ctx] = v[tok:].astype(BF16)

    def kva_copy(i):
        return remote(
            kv_send.at[0, i], kvb.at[g, f], kva_ss.at[0, i], kv_rs.at[me], sp=chip(g, i)
        )

    def kvn_copy(i, slot):
        return remote(
            kv_send.at[1, i, main],
            kvb.at[beside, slot, main],
            kva_ss.at[1, i],
            kv_rs.at[chip(beside, slot)],
            sp=chip(g, i),
        )

    def kvz_copy(way, plane, i, slot):
        peer = me + fan if way == 0 else me - fan
        return remote(
            kvb.at[plane, i], kvb.at[plane, i], kvz_ss.at[slot], kv_rs.at[chip(plane, i)], sp=peer
        )

    def cxz_copy(way, i):
        peer = me + fan if way == 0 else me - fan
        return remote(kvb.at[g, i, extra], kvb.at[g, i, extra], cx_ss.at[i], cx_rs.at[i], sp=peer)

    def pass_own(way, i):
        room = g < planes - 1 if way == 0 else g > 0
        short = send_up if way == 0 else send_down

        @pl.when(room & jnp.logical_not(short))
        def _():
            kvz_copy(way, g, i, chip(g, i) if way == 0 else n_sp + i).start()

        @pl.when(short)
        def _():
            cxz_copy(way, i).start()

    def pass_on(way, plane, i):
        kvz_copy(way, plane, i, chip(plane, i)).start()

    def block_wait(plane, i):
        kvz_copy(0, plane, i, 0).wait_recv()

    def project_kv(i, dst):
        put_kv(jnp.dot(xn[...], wkv[i], preferred_element_type=F32), dst, cosine, sine)

    project_kv(f, kvb.at[g, f])
    pass_own(0, f)
    pass_own(1, f)
    for d in range(1, fan):
        i = lax.rem(f + d, fan)
        project_kv(i, kv_send.at[0, i])
        kva_copy(i).start()

    for copy in loads:
        copy.wait()
    factor = math.log2(math.e) / math.sqrt(hd)

    def project_q(i, dst):
        if fan == 1:
            w = wq[...]
        else:
            w = wq[:, pl.ds(pl.multiple_of(i * qw, qw), qw)]
        q = jnp.dot(xn[0:tok], w, preferred_element_type=F32)
        for h in range(group):
            v = head_rms(q[:, h * hd : (h + 1) * hd], query_gain[...] * factor)
            dst[h * tok : (h + 1) * tok] = rotate(v, cosine, sine).astype(BF16)

    def q_copy(i, slot):
        return remote(q_send.at[i], qb.at[slot], q_ss.at[i], q_rs.at[slot], sp=chip(g, i))

    def before(n):
        return lax.rem(f + fan - n, fan) if fan > 1 else 0

    def after(n):
        return lax.rem(f + 1 + n, fan) if fan > 1 else 0

    for d in range(1, fan):
        i = lax.rem(f + d, fan)
        project_q(i, q_send.at[i])
        q_copy(i, f).start()
        j = before(d)
        block_wait(g, j)
        pass_own(0, j)
        pass_own(1, j)
    project_q(f, qb.at[f])

    def forward(d, slot):
        peer = lax.rem(mt + d, n_tp)
        return remote(lat_next.at[mt], lat_next.at[slot], ln_ss.at[d], ln_rs.at[slot], tp=peer)

    if early:

        @pl.when(edge)
        def _():
            next_copy(0).wait_recv()
            for d in range(1, n_tp):
                forward(d, mt).start()
            cosine, sine = turns(chip(beside, f))
            for d in range(1, n_tp):
                forward(d, lax.rem(mt + d, n_tp)).wait_recv()
            modulate(lat_next, [inverse(lat_next[t].astype(F32)) for t in range(n_tp)])

            def project(i, dst):
                both = jnp.dot(xn[0:tok], wkv[i], preferred_element_type=F32)
                put_kv(both, dst, cosine, sine)

            for d in range(1, fan):
                i = lax.rem(f + d, fan)
                project(i, kv_send.at[1, i])
                kvn_copy(i, f).start()
            project(f, kvb.at[beside, f])

    def beside_wait(i):
        @pl.when(i != f)
        def _():
            kvn_copy(i, i).wait_recv()

        cxz_copy(0, i).wait_recv()

    def arrive(t, n):
        i = before(n)
        inner = jnp.logical_not(edge)

        @pl.when(inner & (g - t >= 0))
        def _():
            block_wait(g - t, i)
            pass_on(0, g - t, i)

        @pl.when(inner & (g + t < planes))
        def _():
            block_wait(g + t, i)
            pass_on(1, g + t, i)

    ahead = min(2, fan)
    for n in range(ahead):
        arrive(1, n)
    for n in range(1, fan):
        q_copy(f, before(n)).wait_recv()

    lift = math.log2(tok * n_sp / (4.0 * ctx * n_sp))
    contract = (((1,), (1,)), ((), ()))
    ones = jnp.ones((ONES, tok), BF16)

    def score(q, parts, buf, peak):
        best = None
        for at, n, key, _, add in parts:
            s = lax.dot_general(key(), q, contract, preferred_element_type=F32)
            if add:
                s = s + add
            buf[at : at + n] = s
            top8 = jnp.max(s.reshape(n // 8, 8, wide), axis=0)
            best = top8 if best is None else jnp.maximum(best, top8)
        peak[...] = jnp.max(best, axis=0, keepdims=True)

    def finish(i, parts, buf, peak):
        old = m_ref[i]
        new = jnp.maximum(peak[...], old)
        m_ref[i] = new
        total = None
        for at, n, _, value, _ in parts:
            e = jnp.exp2(buf[at : at + n] - new).astype(BF16)
            v = jnp.concatenate([value(), ones[:, :n]], axis=0)
            p = jnp.dot(v, e, preferred_element_type=F32)
            total = p if total is None else total + p
        acc_ref[i] = acc_ref[i] * jnp.exp2(old - new) + total

    def chunk_value(plane, c):
        return jnp.concatenate(
            [kvb[plane, c, tok + j * hd : tok + (j + 1) * hd] for j in range(tok // hd)], axis=1
        )

    def chunk_parts(plane, chunks):
        parts = []
        for k, c in enumerate(chunks):
            parts.append(
                (
                    k * tok,
                    tok,
                    lambda c=c: kvb[plane, c, 0:tok],
                    lambda c=c: chunk_value(plane, c),
                    0.0,
                )
            )
        ckey = jnp.concatenate([kvb[plane, c, 2 * tok : 2 * tok + ctx] for c in chunks], axis=0)
        cval = jnp.concatenate(
            [kvb[plane, c, 2 * tok + ctx : 2 * tok + 2 * ctx] for c in chunks], axis=0
        )
        cval = cval.astype(F32).T.astype(BF16)
        n = len(chunks) * ctx
        parts.append((len(chunks) * tok, n, lambda: ckey, lambda: cval, lift))
        return parts

    bufs = ((s0, n0), (s1, n1))

    def attend(parts, order, done):
        score(qb[order[0]], parts, *bufs[0])
        for k, i in enumerate(order):
            if k + 1 < len(order):
                score(qb[order[k + 1]], parts, *bufs[(k + 1) % 2])
            finish(i, parts, *bufs[k % 2])
            done(k, i)

    def nothing(k, i):
        pass

    all_groups = list(range(fan))

    @pl.loop(0, 2 * planes - 3)
    def _(v):
        t = lax.div(v + 1, 2)
        down = lax.rem(v, 2) == 1
        plane = jnp.where(down, g - t, g + t)
        valid = (plane >= 0) & (plane < planes)

        @pl.when(valid & edge & (v > 0))
        def _():
            @pl.when((t == 1) & early)
            def _():
                for n in range(fan):
                    beside_wait(before(n))

            @pl.when(jnp.logical_not((t == 1) & early))
            def _():
                for n in range(fan):
                    block_wait(plane, before(n))

        @pl.when(valid)
        def _():
            attend(chunk_parts(plane, all_groups), all_groups, nothing)

        @pl.when(down)
        def _():
            arrive(t + 1, 0)

        for n in range(1, fan):

            @pl.when(jnp.logical_not(down) & ((v > 0) | (n >= ahead)))
            def _():
                arrive(t + 1, n)

    def at_copy(i, slot):
        return remote(
            att_send.at[i], att_recv.at[slot], at_ss.at[i], at_rs.at[slot], sp=chip(g, i)
        )

    def give(n, i):
        a = acc_ref[i]
        a = a[:hd] * (1.0 / a[hd : hd + 1])
        heads = [a[:, h * tok : (h + 1) * tok].T.astype(BF16) for h in range(group)]
        dst = att_send.at[i] if n < fan - 1 else att_recv.at[f]
        for h in range(group):
            dst[:, h * hd : (h + 1) * hd] = heads[h]
        if n < fan - 1:
            at_copy(i, f).start()

    targets = [after(n) for n in range(fan)]

    @pl.when(edge)
    def _():
        far = jnp.where(bottom, planes - 1, 0)

        @pl.loop(0, fan - 1)
        def _(d):
            j = before(d)
            block_wait(far, j)
            attend(chunk_parts(far, [j]), all_groups, nothing)

        j = before(fan - 1)
        block_wait(far, j)
        attend(chunk_parts(far, [j]), targets, give)

    @pl.when(jnp.logical_not(edge))
    def _():
        for n in range(fan):
            give(n, targets[n])

    wait_all(gate_recv, red_sem.at[3])
    gate_all[mt] = lax.fori_loop(1, n_sp, lambda i, s: s + gate_recv[i], gate_recv[0])

    def ga_copy(d, slot):
        peer = lax.rem(mt + d, n_tp)
        return remote(gate_all.at[mt], gate_all.at[slot], ga_ss.at[d], ga_rs.at[slot], tp=peer)

    for d in range(1, n_tp):
        ga_copy(d, mt).start()
    out_load.wait()

    def out_rows(i):
        return wo[pl.ds(pl.multiple_of(i * qw, qw), qw)] if fan > 1 else wo[...]

    def project_out(t, i):
        r = pl.ds(pl.multiple_of(t * rows, rows), rows)
        p = jnp.dot(att_recv[i, r], out_rows(i), preferred_element_type=F32)
        return (psum[r] + p if fan > 1 else p).astype(BF16)

    if fan > 1:
        psum[...] = jnp.dot(att_recv[f], out_rows(f), preferred_element_type=F32)
    for n in range(1, fan - 1):
        i = before(n)
        at_copy(f, i).wait_recv()
        psum[...] += jnp.dot(att_recv[i], out_rows(i), preferred_element_type=F32)
    last = before(fan - 1)
    if fan > 1:
        at_copy(f, last).wait_recv()

    def pt_copy(d, t, slot):
        return remote(part_send.at[t], part_recv.at[slot], pt_ss.at[t], pt_rs.at[slot], tp=t)

    for d in range(1, n_tp):
        t = lax.rem(mt + d, n_tp)
        part_send[t] = project_out(t, last)
        pt_copy(d, t, mt).start()
    part_recv[mt] = project_out(mt, last)
    for d in range(1, n_tp):
        ga_copy(d, lax.rem(mt + d, n_tp)).wait_recv()
    for d in range(1, n_tp):
        t = lax.rem(mt + d, n_tp)
        pt_copy(d, t, t).wait_recv()
    mixed = part_recv[0].astype(F32)
    for t in range(1, n_tp):
        mixed = mixed + part_recv[t].astype(F32)
    inv = lax.rsqrt(jnp.mean(mixed * mixed, axis=-1, keepdims=True) + EPS)
    for t in range(n_tp):
        cols = slice(t * width, (t + 1) * width)
        out[:, cols] = (
            latent[:, cols].astype(F32)
            + gate_all[t] * (mixed[:, cols] * inv * post_gain[:, cols])
        ).astype(BF16)

    wait_all(mod_recv, red_sem.at[0])
    wait_all(gate_recv, red_sem.at[2])

    for d in range(1, n_tp):
        lat_copy(d, mt).wait_send()
        ma_copy(d, mt).wait_send()
        ga_copy(d, mt).wait_send()
        t = lax.rem(mt + d, n_tp)
        pt_copy(d, t, mt).wait_send()
    for d in range(1, fan):
        i = lax.rem(f + d, fan)
        kva_copy(i).wait_send()
        q_copy(i, f).wait_send()
        at_copy(i, f).wait_send()

    if early:

        @pl.when(send_up)
        def _():
            next_copy(0).wait_send()

        @pl.when(send_down)
        def _():
            next_copy(1).wait_send()

        @pl.when(edge)
        def _():
            for d in range(1, n_tp):
                forward(d, mt).wait_send()
            for d in range(1, fan):
                kvn_copy(lax.rem(f + d, fan), f).wait_send()

    for i in range(fan):

        @pl.when((g < planes - 1) & jnp.logical_not(send_up))
        def _():
            kvz_copy(0, g, i, chip(g, i)).wait_send()

        @pl.when((g > 0) & jnp.logical_not(send_down))
        def _():
            kvz_copy(1, g, i, n_sp + i).wait_send()

        @pl.when(send_up | send_down)
        def _():
            cxz_copy(0, i).wait_send()

    @pl.when(jnp.logical_not(edge))
    def _():
        @pl.loop(0, planes)
        def _(plane):
            @pl.when(plane != g)
            def _():
                for i in range(fan):
                    kvz_copy(0, plane, i, chip(plane, i)).wait_send()


def body(
    latent,
    condition,
    context_condition,
    context,
    w_shift,
    w_scale,
    w_gate,
    pre_gain,
    post_gain,
    query_gain,
    key_gain,
    w_query,
    w_key,
    w_value,
    w_out,
):
    n_sp = lax.axis_size("sp")
    n_tp = lax.axis_size("tp")
    hd = query_gain.shape[0]
    kv_dev = w_key.shape[1] // hd
    group = w_query.shape[1] // w_key.shape[1]
    fan = kv_dev
    planes = n_sp // fan
    rows, depth = latent.shape
    tok = rows * n_tp
    ctx = context.shape[0]
    width = w_shift.shape[1]
    sizes = (n_sp, n_tp, fan, planes, group, hd, tok, rows, ctx)
    chunk = 2 * tok + 2 * ctx
    keys = fan * (tok + ctx)
    wide = group * tok
    vmem = pl.BlockSpec(memory_space=pltpu.VMEM)
    hbm = pl.BlockSpec(memory_space=pl.ANY)
    dma = pltpu.SemaphoreType.DMA
    scratch = [
        pltpu.VMEM(w_query.shape, BF16),
        pltpu.VMEM((fan, depth, 2 * hd), BF16),
        pltpu.VMEM(w_out.shape, BF16),
        pltpu.VMEM((n_tp, rows, depth), BF16),
        pltpu.VMEM((n_tp, rows, depth), BF16),
        pltpu.VMEM((4, width), F32),
        pltpu.VMEM((n_sp, 4, width), F32),
        pltpu.VMEM((1, width), F32),
        pltpu.VMEM((n_sp, 1, width), F32),
        pltpu.VMEM((n_tp, 4, width), F32),
        pltpu.VMEM((n_tp, 1, width), F32),
        pltpu.VMEM((tok + ctx, depth), BF16),
        pltpu.VMEM((2, fan, chunk, hd), BF16),
        pltpu.VMEM((fan, wide, hd), BF16),
        pltpu.VMEM((planes, fan, chunk, hd), BF16),
        pltpu.VMEM((fan, wide, hd), BF16),
        pltpu.VMEM((fan, 1, wide), F32),
        pltpu.VMEM((fan, hd + ONES, wide), F32),
        pltpu.VMEM((keys, wide), F32),
        pltpu.VMEM((keys, wide), F32),
        pltpu.VMEM((1, wide), F32),
        pltpu.VMEM((1, wide), F32),
        pltpu.VMEM((fan, tok, group * hd), BF16),
        pltpu.VMEM((fan, tok, group * hd), BF16),
        pltpu.VMEM((tok, depth), F32),
        pltpu.VMEM((n_tp, rows, depth), BF16),
        pltpu.VMEM((n_tp, rows, depth), BF16),
        dma((2 + 2 * fan,)),
        dma((n_tp,)),
        dma((n_tp,)),
        dma((n_tp,)),
        dma((n_tp,)),
        dma((2,)),
        dma((4,)),
        dma((n_tp,)),
        dma((n_tp,)),
        dma((n_tp,)),
        dma((n_tp,)),
        dma((2, fan)),
        dma((n_sp + fan,)),
        dma((n_sp,)),
        dma((fan,)),
        dma((fan,)),
        dma((fan,)),
        dma((fan,)),
        dma((fan,)),
        dma((fan,)),
        dma((n_tp,)),
        dma((n_tp,)),
    ]
    return pl.pallas_call(
        functools.partial(kernel, sizes),
        out_shape=jax.ShapeDtypeStruct(latent.shape, BF16),
        in_specs=[vmem] * 11 + [hbm] * 4,
        out_specs=vmem,
        scratch_shapes=scratch,
        compiler_params=pltpu.CompilerParams(
            collective_id=0, has_side_effects=True, vmem_limit_bytes=60 * 1024 * 1024
        ),
    )(
        latent,
        condition.reshape(1, -1),
        context_condition.reshape(1, -1),
        context,
        w_shift,
        w_scale,
        w_gate,
        pre_gain.reshape(1, -1),
        post_gain.reshape(1, -1),
        query_gain.reshape(1, -1),
        key_gain.reshape(1, -1),
        w_query,
        w_key,
        w_value,
        w_out,
    )


def solution(mesh):
    placed = (
        P(("sp", "tp"), None),
        P("sp"),
        P("sp"),
        P("sp", None),
        P("sp", "tp"),
        P("sp", "tp"),
        P("sp", "tp"),
        P(),
        P(),
        P(),
        P(),
        P(None, "tp"),
        P(None, "tp"),
        P(None, "tp"),
        P("tp", None),
    )
    return jax.shard_map(
        body, mesh=mesh, in_specs=placed, out_specs=P(("sp", "tp"), None), check_vma=False
    )
```
